32 devices in a mesh: kv: 8 (over y, x, core), tp: 4 (over z).
Axes of the slice: x: 2, y: 2, z: 4, core: 2. Of those that a mesh axis runs over, the one named last changes fastest.
Arguments:
- tokens: bfloat16 [320, 4096], P('tp', 'kv'), may hold values from -8 to 8
- state: float32 [320, 32, 128, 128], P('kv', 'tp'), may hold values from -4 to 4
- mix_gain: float32 [4096], P('kv'), may hold values from 0.1 to 1.9
- q_weight: bfloat16 [4096, 4096], P('kv', 'tp'), may hold values from -0.09375 to 0.09375
- forget_weight: bfloat16 [4096, 4096], P('kv', 'tp'), may hold values from -0.09375 to 0.09375
- input_weight: bfloat16 [4096, 4096], P('kv', 'tp'), may hold values from -0.09375 to 0.09375
- gate_weight: bfloat16 [4096, 4096], P('kv', 'tp'), may hold values from -0.09375 to 0.09375
- lower_bound: float32 [4096], P('tp'), may hold values from 0 to 0.9
- head_gain: float32 [128], replicated, may hold values from 0.1 to 1.9
- out_weight: bfloat16 [4096, 4096], P('tp', 'kv'), may hold values from -0.09375 to 0.09375
- ffn_gain: float32 [4096], P('kv'), may hold values from 0.1 to 1.9
- ffn_gate: bfloat16 [4096, 10240], P('kv', 'tp'), may hold values from -0.09375 to 0.09375
- ffn_up: bfloat16 [4096, 10240], P('kv', 'tp'), may hold values from -0.09375 to 0.09375
- ffn_down: bfloat16 [10240, 4096], P('tp', 'kv'), may hold values from -0.0625 to 0.0625
Outputs:
- layer_out: bfloat16 [320, 4096], P('tp', 'kv')
- new_state: float32 [320, 32, 128, 128], P('kv', 'tp')
The draws below stay inside these ranges and needn't reach their ends.
All inputs are finite; a program needn't handle non-finite values.
Results may differ from the reference program's by a relative error of at most 0.007.
Values may be sent and summed in bfloat16 or wider, within the bound.
No kernel may reach another device: no remote copies, remote signals or barrier semaphores. Data moves between devices by JAX's collectives and lax.ppermute only.
A program may use at most 128 MiB of HBM per device.

```python
import jax
import jax.numpy as jnp
from jax import lax

HEADS = 32
HEAD = 128
D = 4096
FF = 10240
BATCH = 320


def draw_tokens(key, part):
    first, second, third, fourth = jax.random.split(jax.random.fold_in(key, 17), 4)
    base = jax.random.normal(first, (BATCH, D), jnp.float32)
    block_scale = jnp.exp(jax.random.uniform(second, (32,), jnp.float32, -1.2, 1.2))
    column_scale = jnp.repeat(block_scale, D // 32)
    values = base * column_scale[None, :]
    return jnp.clip(values, -8.0, 8.0).astype(jnp.bfloat16)


def levels(stream_key, shape, cuts, least, top_value):
    def one(axis_at, parts):
        draws = jax.random.uniform(jax.random.fold_in(jax.random.fold_in(stream_key, 6), axis_at), (parts,), jnp.float32, least / len(cuts), top_value / len(cuts))
        return jnp.repeat(jnp.exp(draws), shape[axis_at] // parts).reshape((-1,) + (1,) * (len(shape) - axis_at - 1))

    loudness = one(*cuts[0])
    for cut in cuts[1:]:
        loudness = loudness * one(*cut)
    return loudness


def gaussian(key, shape, scale, bound, shards=(), kind=jnp.bfloat16):
    array = scale * jax.random.normal(key, shape, jnp.float32)
    if shards:
        array = array * levels(key, shape, shards, -0.22, 0.18)
    return jnp.clip(array, -bound, bound).astype(kind)


def setup_inputs(seed: int = 0) -> dict:
    key_of = jax.random.split(jax.random.key(seed), 15)
    tokens = draw_tokens(jax.random.fold_in(key_of[14], 71), 0)
    state = gaussian(key_of[1], (BATCH, HEADS, HEAD, HEAD), 0.5, 4.0, ((0, 8), (1, 4)), jnp.float32)
    mix_gain = jnp.clip(1.0 + 0.18 * jax.random.normal(key_of[2], (D,), jnp.float32), 0.1, 1.9)
    q_weight = gaussian(key_of[3], (D, D), D ** -0.5, 0.09375, ((0, 8), (1, 4)))
    forget_weight = gaussian(key_of[4], (D, D), D ** -0.5, 0.09375, ((0, 8), (1, 4)))
    input_weight = gaussian(key_of[5], (D, D), D ** -0.5, 0.09375, ((0, 8), (1, 4)))
    gate_weight = gaussian(key_of[6], (D, D), D ** -0.5, 0.09375, ((0, 8), (1, 4)))
    lower_bound = jnp.clip(0.9 * jax.random.uniform(key_of[7], (D,), jnp.float32) ** levels(key_of[7], (D,), ((0, 4),), -0.2, 0.2), 0.0, 0.9)
    head_gain = jnp.clip(1.0 + 0.18 * jax.random.normal(key_of[8], (HEAD,), jnp.float32), 0.1, 1.9)
    out_weight = gaussian(key_of[9], (D, D), D ** -0.5, 0.09375, ((0, 4), (1, 8)))
    ffn_gain = jnp.clip(1.0 + 0.18 * jax.random.normal(key_of[10], (D,), jnp.float32), 0.1, 1.9)
    ffn_gate = gaussian(key_of[11], (D, FF), D ** -0.5, 0.09375, ((0, 8), (1, 4)))
    ffn_up = gaussian(key_of[12], (D, FF), D ** -0.5, 0.09375, ((0, 8), (1, 4)))
    ffn_down = gaussian(key_of[13], (FF, D), FF ** -0.5, 0.0625, ((0, 4), (1, 8)))
    return {"tokens": tokens, "state": state, "mix_gain": mix_gain, "q_weight": q_weight, "forget_weight": forget_weight, "input_weight": input_weight, "gate_weight": gate_weight, "lower_bound": lower_bound, "head_gain": head_gain, "out_weight": out_weight, "ffn_gain": ffn_gain, "ffn_gate": ffn_gate, "ffn_up": ffn_up, "ffn_down": ffn_down}


EPS = 1e-05

def reference(tokens, state, mix_gain, q_weight, forget_weight, input_weight, gate_weight, lower_bound, head_gain, out_weight, ffn_gain, ffn_gate, ffn_up, ffn_down):
    batch_rows = tokens.shape[0]
    values = tokens.astype(jnp.float32)
    factor = lax.rsqrt(lax.optimization_barrier(jnp.mean(values * values, axis=1, keepdims=True)) + EPS)
    normed = (values * mix_gain).astype(jnp.bfloat16)

    def project(weight):
        return jnp.dot(normed, weight, preferred_element_type=jnp.float32) * factor
    query_pre = project(q_weight)
    forget_pre = project(forget_weight)
    value_pre = project(input_weight)
    gate_pre = project(gate_weight)
    split_shape = (batch_rows, HEADS, HEAD)
    query = (jax.nn.silu(query_pre) * HEAD ** (-0.5)).reshape(split_shape)
    forget = (lower_bound + (1.0 - lower_bound) * jax.nn.sigmoid(forget_pre)).reshape(split_shape)
    value = value_pre.reshape(split_shape)
    new_state = forget[..., None] * state + (1.0 - forget)[..., None] * value[:, :, None, :]
    read = jnp.einsum('bhk,bhkv->bhv', query, new_state, precision=lax.Precision.HIGHEST)
    read = read * lax.rsqrt(lax.optimization_barrier(jnp.mean(read * read, axis=-1, keepdims=True)) + EPS) * head_gain
    gated = (read.reshape(batch_rows, D) * jax.nn.silu(gate_pre)).astype(jnp.bfloat16)
    residual = (values + jnp.dot(gated, out_weight, preferred_element_type=jnp.float32)).astype(jnp.bfloat16)
    res_values = residual.astype(jnp.float32)
    factor_ffn = lax.rsqrt(lax.optimization_barrier(jnp.mean(res_values * res_values, axis=1, keepdims=True)) + EPS)
    normed_ffn = (res_values * ffn_gain).astype(jnp.bfloat16)
    gate_ffn = jnp.dot(normed_ffn, ffn_gate, preferred_element_type=jnp.float32) * factor_ffn
    up_ffn = jnp.dot(normed_ffn, ffn_up, preferred_element_type=jnp.float32) * factor_ffn
    hidden = (jax.nn.silu(gate_ffn) * up_ffn).astype(jnp.bfloat16)
    layer_out = (res_values + jnp.dot(hidden, ffn_down, preferred_element_type=jnp.float32)).astype(jnp.bfloat16)
    return (layer_out, new_state)
```

```python
import jax
import jax.numpy as jnp
from jax import lax
from jax.experimental import pallas as pl
from jax.experimental.pallas import tpu as pltpu
from jax.sharding import PartitionSpec as P

EPS = 1e-05
STREAMS = 1
HEADS_STEP = 8
F32 = jnp.float32
BF16 = jnp.bfloat16


def swap(x, distance, axis):
    size = lax.axis_size(axis)
    return lax.ppermute(x, axis, [(i, i ^ distance) for i in range(size)])


def bits_of(size):
    return size.bit_length() - 1


def block_order(bit_sequence):
    order = [0]
    for bit in reversed(bit_sequence):
        order = order + [k | (1 << bit) for k in order]
    return order


def pick_rows(x, source_row):
    here = lax.broadcasted_iota(jnp.int32, (source_row.shape[0], x.shape[0]), 1)
    onehot = (here == source_row[:, None]).astype(BF16)
    return jnp.dot(onehot, x, preferred_element_type=F32).astype(BF16)


def rows_of(blocks, rows):
    return (blocks[:, None] * rows + jnp.arange(rows, dtype=jnp.int32)[None, :]).reshape(-1)


def gather_tp(own):
    return jnp.concatenate(
        [own] + [swap(own, d, "tp") for d in range(1, lax.axis_size("tp"))], axis=0
    )


def gather_kv(own):
    near = [own] + [swap(own, d, "kv") for d in range(2, lax.axis_size("kv"), 2)]
    near = jnp.stack(near, axis=0)
    return near, swap(near, 1, "kv")


def gather_kv_order():
    even = list(range(0, lax.axis_size("kv"), 2))
    return even + [k | 1 for k in even]


LANES = 128


def project_in(own, gain, weights, width):
    kv_size, tp_size = lax.axis_size("kv"), lax.axis_size("tp")
    me_kv, me_tp = lax.axis_index("kv"), lax.axis_index("tp")
    tp_rows = own.shape[0]
    total = tp_rows * tp_size
    kv_rows = total // kv_size
    everyone = gather_tp(own)
    bits = bits_of(kv_size)

    def where(rows):
        return ((rows // tp_rows) ^ me_tp) * tp_rows + rows % tp_rows

    ordered = {}
    results = []
    parts = []
    half = total // 2
    for at, weight in enumerate(weights):
        turn = at % max(bits - 1, 1)
        rest = list(range(1, bits))
        sequence = tuple([0] + rest[turn:] + rest[:turn])
        if sequence not in ordered:
            blocks = me_kv ^ jnp.array(block_order(sequence), jnp.int32)
            moved = pick_rows(everyone, where(rows_of(blocks, kv_rows))).astype(F32)
            ordered[sequence] = (moved * gain).astype(BF16)
        rows = ordered[sequence]
        away = jnp.dot(rows[half:], weight, preferred_element_type=F32).astype(BF16)
        squares = None
        if at == 0:
            squares = jnp.sum(moved * moved, axis=1, keepdims=True)
            squares = jnp.broadcast_to(squares, (total, LANES))
            away = jnp.concatenate([away, squares[half:].astype(BF16)], axis=1)
            squares = squares[:half]
        parts.append((sequence, rows[:half], weight, squares, swap(away, 1, "kv")))
    for sequence, rows, weight, squares, came in parts:
        kept = jnp.dot(rows, weight, preferred_element_type=F32)
        if squares is not None:
            kept = jnp.concatenate([kept, squares], axis=1)
        for bit in sequence[1:]:
            partial = (kept + came.astype(F32)).astype(BF16)
            cut = partial.shape[0] // 2
            came = swap(partial[cut:], 1 << bit, "kv")
            kept = partial[:cut].astype(F32)
        results.append(kept + came.astype(F32))
    columns = weights[0].shape[1]
    factor = lax.rsqrt(results[0][:, columns : columns + 1] / width + EPS)
    results[0] = results[0][:, :columns]
    return [r * factor for r in results]


def project_back(own, weight):
    kv_size, tp_size = lax.axis_size("kv"), lax.axis_size("tp")
    me_kv, me_tp = lax.axis_index("kv"), lax.axis_index("tp")
    kv_rows = own.shape[0]
    total = kv_rows * kv_size
    tp_rows = total // tp_size
    partial = jnp.concatenate(
        [
            jnp.einsum("nrc,cd->nrd", rows, weight, preferred_element_type=F32).astype(BF16)
            for rows in gather_kv(own)
        ],
        axis=0,
    ).reshape(total, weight.shape[1])
    order = gather_kv_order()
    place = jnp.array([order.index(k) for k in range(kv_size)], jnp.int32)
    wanted = rows_of(me_tp ^ jnp.arange(tp_size, dtype=jnp.int32), tp_rows)
    relative = (wanted // kv_rows) ^ me_kv
    onehot = relative[:, None] == jnp.arange(kv_size, dtype=jnp.int32)[None, :]
    slot = jnp.sum(jnp.where(onehot, place[None, :], 0), axis=1)
    partial = pick_rows(partial, slot * kv_rows + wanted % kv_rows)
    total_sum = partial[:tp_rows].astype(F32)
    for d in range(1, tp_size):
        total_sum = total_sum + swap(partial[d * tp_rows : (d + 1) * tp_rows], d, "tp").astype(F32)
    return total_sum


def state_step(q_ref, f_ref, v_ref, g_ref, bound_ref, gain_ref, state_ref, *rest):
    new_ref, gated_ref = rest[-2:]
    rows, heads, size = state_ref.shape[0], state_ref.shape[1], state_ref.shape[2]
    gain = gain_ref[...]
    for h in range(heads):
        cols = slice(h * size, (h + 1) * size)
        q = q_ref[0, :, cols]
        q = q * jax.nn.sigmoid(q) * size ** (-0.5)
        bound = bound_ref[:, cols]
        f = bound + (1.0 - bound) * jax.nn.sigmoid(f_ref[0, :, cols])
        q_cols, f_cols = q.T, f.T
        v = v_ref[0, :, cols]
        reads = []
        for b in range(rows):
            v_row = v[b : b + 1, :]
            updated = v_row + f_cols[:, b : b + 1] * (state_ref[b, h] - v_row)
            new_ref[b, h] = updated
            reads.append(jnp.sum(q_cols[:, b : b + 1] * updated, axis=0, keepdims=True))
        read = jnp.concatenate(reads, axis=0)
        read = read * lax.rsqrt(jnp.mean(read * read, axis=1, keepdims=True) + EPS) * gain
        g = g_ref[0, :rows, cols]
        gated_ref[0, :, cols] = read * (g * jax.nn.sigmoid(g))


def update_state(sums, bound, gain, state, stream, previous):
    rows, cols = sums[0].shape
    heads, size = state.shape[1], state.shape[2]
    block = max(b for b in range(1, 9) if rows % b == 0)
    steps = rows // block
    split = [s.reshape(steps, block, cols) for s in sums]
    if block < 8:
        split = [jnp.pad(s, ((0, 0), (0, 8 - block), (0, 0))) for s in split]
    first = stream * steps
    some = max(h for h in range(1, HEADS_STEP + 1) if heads % h == 0)
    wide = some * size
    vec = pl.BlockSpec((1, 8, wide), lambda i, j: (i, 0, j))
    big = pl.BlockSpec((block, some, size, size), lambda i, j: (first + i, j, 0, 0))
    operands = [*split, bound[None, :], gain[None, :], state]
    specs = [vec] * 4 + [
        pl.BlockSpec((1, wide), lambda i, j: (0, j)),
        pl.BlockSpec((1, size), lambda i, j: (0, 0)),
        big,
    ]
    aliases = {}
    if previous is not None:
        aliases = {len(operands): 0}
        operands.append(previous)
        specs.append(pl.BlockSpec(memory_space=pl.ANY))
    new_state, gated = pl.pallas_call(
        state_step,
        grid=(steps, heads // some),
        in_specs=specs,
        out_specs=[big, pl.BlockSpec((1, block, wide), lambda i, j: (i, 0, j))],
        out_shape=[
            jax.ShapeDtypeStruct(state.shape, F32),
            jax.ShapeDtypeStruct((steps, block, cols), F32),
        ],
        input_output_aliases=aliases,
        compiler_params=pltpu.CompilerParams(dimension_semantics=("arbitrary", "arbitrary")),
        name="state_step",
    )(*operands)
    return new_state, gated.reshape(rows, cols).astype(BF16)


def body(
    tokens,
    state,
    mix_gain,
    q_weight,
    forget_weight,
    input_weight,
    gate_weight,
    lower_bound,
    head_gain,
    out_weight,
    ffn_gain,
    ffn_gate,
    ffn_up,
    ffn_down,
):
    width = tokens.shape[1] * lax.axis_size("kv")
    kv_rows = state.shape[0]
    tp_rows = tokens.shape[0]
    streams = STREAMS
    blocks = tp_rows // kv_rows
    pieces = tokens.reshape(blocks, streams, kv_rows // streams, tokens.shape[1])
    new_state = None
    outs = []
    for s in range(streams):
        own = pieces[:, s].reshape(tp_rows // streams, tokens.shape[1])
        sums = project_in(own, mix_gain, (q_weight, forget_weight, input_weight, gate_weight), width)
        new_state, gated = update_state(sums, lower_bound, head_gain, state, s, new_state)
        residual = (own.astype(F32) + project_back(gated, out_weight)).astype(BF16)
        gate, up = project_in(residual, ffn_gain, (ffn_gate, ffn_up), width)
        hidden = (jax.nn.silu(gate) * up).astype(BF16)
        out = (residual.astype(F32) + project_back(hidden, ffn_down)).astype(BF16)
        outs.append(out.reshape(blocks, 1, kv_rows // streams, tokens.shape[1]))
    layer_out = jnp.concatenate(outs, axis=1).reshape(tokens.shape)
    return (layer_out, new_state)


def solution(mesh):
    in_specs = (
        P("tp", "kv"),
        P("kv", "tp", None, None),
        P("kv"),
        P("kv", "tp"),
        P("kv", "tp"),
        P("kv", "tp"),
        P("kv", "tp"),
        P("tp"),
        P(),
        P("tp", "kv"),
        P("kv"),
        P("kv", "tp"),
        P("kv", "tp"),
        P("tp", "kv"),
    )
    out_specs = (P("tp", "kv"), P("kv", "tp", None, None))
    return jax.shard_map(body, mesh=mesh, in_specs=in_specs, out_specs=out_specs, check_vma=False)
```
